32 devices in a mesh: sp: 8 (over z, y), tp: 4 (over x, core).
Axes of the slice: x: 2, y: 2, z: 4, core: 2. Of those that a mesh axis runs over, the one named last changes fastest.
Arguments:
- tokens: bfloat16 [1024, 2048], P(('sp', 'tp')), may hold values from -64 to 64, as said below
- query_one: bfloat16 [2048, 256], P(None, 'tp'), may hold values from -0.125 to 0.125
- query_two: bfloat16 [2048, 256], P(None, 'tp'), may hold values from -0.125 to 0.125
- key_one: bfloat16 [2048, 256], P(None, 'tp'), may hold values from -0.125 to 0.125
- key_two: bfloat16 [2048, 256], P(None, 'tp'), may hold values from -0.125 to 0.125
- value_weight: bfloat16 [2048, 512], P(None, 'tp'), may hold values from -0.125 to 0.125
- mixing: float32 [4], P('tp'), may hold values from 0.3 to 0.8
- out_weight: bfloat16 [512, 2048], replicated, may hold values from -0.25 to 0.25
- head_gain: float32 [128], replicated, may hold values from 0.1 to 1.9
Outputs:
- attended: bfloat16 [1024, 2048], P(('sp', 'tp'))
The draws below stay inside these ranges and needn't reach their ends.
Inputs may be any that keep to these rules, and one draw needn't show every extreme that they name: `tokens`: Real-valued activations.
All inputs are finite; a program needn't handle non-finite values.
Results may differ from the reference program's by a relative error of at most 0.012.
The reference program's roundings to bfloat16 on the way count: a program that leaves them out, or rounds other values in their place, can miss the bound.
Values may be sent and summed in bfloat16 or wider, within the bound.
No kernel may reach another device: no remote copies, remote signals or barrier semaphores. Data moves between devices by JAX's collectives and lax.ppermute only.
A program may use at most 64 MiB of HBM per device.

```python
import math
import jax
import jax.numpy as jnp
from jax import lax

D = 2048
HEADS = 4
HEAD = 64
GRID_W = 64
TOK_DEV = 128
TOKENS = 1024


def draw_tokens(key, part):
    key_base = jax.random.fold_in(key, 11)
    key_means = jax.random.fold_in(key, 12)
    blocks = TOKENS // TOK_DEV
    means = jnp.clip(jax.random.normal(key_means, (blocks, D), jnp.float32), -4.0, 4.0)
    spread_means = jnp.repeat(means, TOK_DEV, axis=0)
    base = jnp.clip(jax.random.normal(key_base, (TOKENS, D), jnp.float32), -4.0, 4.0)
    field = base + spread_means
    return jnp.clip(field, -64.0, 64.0).astype(jnp.bfloat16)


def level_of(rng, extent, shards, low, high):
    gain = 1.0
    for axis_at, parts in shards:
        heights = jax.random.uniform(jax.random.fold_in(jax.random.fold_in(rng, 6), axis_at), (parts,), jnp.float32, low / len(shards), high / len(shards))
        gain = gain * jnp.repeat(jnp.exp(heights), extent[axis_at] // parts).reshape((-1,) + (1,) * (len(extent) - 1 - axis_at))
    return gain


def bell_draw(stream_key, extent, width, reach, cuts=(), held_as=jnp.bfloat16):
    values = width * jax.random.normal(stream_key, extent, jnp.float32)
    if cuts:
        values = values * level_of(stream_key, extent, cuts, -0.22, 0.18)
    return jnp.clip(values, -reach, reach).astype(held_as)


def setup_inputs(seed: int = 0) -> dict:
    key_of = jax.random.split(jax.random.key(seed), 10)
    return {
        "tokens": draw_tokens(jax.random.fold_in(key_of[9], 71), 0),
        "query_one": bell_draw(key_of[1], (D, HEADS * HEAD), D ** -0.5, 0.125, ((1, 4),)),
        "query_two": bell_draw(key_of[2], (D, HEADS * HEAD), D ** -0.5, 0.125, ((1, 4),)),
        "key_one": bell_draw(key_of[3], (D, HEADS * HEAD), D ** -0.5, 0.125, ((1, 4),)),
        "key_two": bell_draw(key_of[4], (D, HEADS * HEAD), D ** -0.5, 0.125, ((1, 4),)),
        "value_weight": bell_draw(key_of[5], (D, HEADS * 2 * HEAD), D ** -0.5, 0.125, ((1, 4),)),
        "mixing": jnp.clip(0.3 + 0.5 * jax.random.uniform(key_of[6], (HEADS,), jnp.float32) ** level_of(key_of[6], (HEADS,), ((0, 4),), -0.2, 0.2), 0.3, 0.8),
        "out_weight": bell_draw(key_of[7], (HEADS * 2 * HEAD, D), (2 * HEADS * HEAD) ** -0.5, 0.25),
        "head_gain": jnp.clip(1.0 + 0.18 * jax.random.normal(key_of[8], (2 * HEAD,), jnp.float32), 0.1, 1.9),
    }


epsilon = 1e-06
theta_base = 10000.0

def grid_turn(field, positions):
    quarter = field.shape[-1] // 4
    half = 2 * quarter
    freqs = theta_base ** (-jnp.arange(quarter, dtype=jnp.float32) / quarter)
    row_angle = (positions // GRID_W).astype(jnp.float32)[:, None] * freqs
    col_angle = (positions % GRID_W).astype(jnp.float32)[:, None] * freqs

    def turn(segment, angle):
        cosine = jnp.cos(angle)[:, None, :]
        sine = jnp.sin(angle)[:, None, :]
        first = segment[..., :quarter]
        second = segment[..., quarter:]
        return jnp.concatenate([first * cosine - second * sine, first * sine + second * cosine], axis=-1)
    return jnp.concatenate([turn(field[..., :half], row_angle), turn(field[..., half:], col_angle)], axis=-1)

def project(tokens, weight):
    product = jnp.dot(tokens, weight, preferred_element_type=jnp.float32)
    return product.reshape(tokens.shape[0], HEADS, -1)

def reference(tokens, query_one, query_two, key_one, key_two, value_weight, mixing, out_weight, head_gain):
    positions = jnp.arange(TOKENS, dtype=jnp.int32)
    q_first = grid_turn(project(tokens, query_one), positions).astype(jnp.bfloat16)
    q_second = grid_turn(project(tokens, query_two), positions).astype(jnp.bfloat16)
    k_first = grid_turn(project(tokens, key_one), positions).astype(jnp.bfloat16).astype(jnp.float32)
    k_second = grid_turn(project(tokens, key_two), positions).astype(jnp.bfloat16).astype(jnp.float32)
    values = project(tokens, value_weight).astype(jnp.bfloat16).astype(jnp.float32)
    scale = HEAD ** (-0.5)
    block_rows = math.gcd(TOKENS, 256)

    def one_map(queries, keys):
        scores = jnp.einsum('qhd,khd->qhk', queries.astype(jnp.float32), keys) * scale
        peak = lax.optimization_barrier(jnp.max(scores, axis=-1, keepdims=True))
        weights = jnp.exp(scores - peak)
        total = lax.optimization_barrier(jnp.sum(weights, axis=-1))
        rounded = lax.optimization_barrier(weights.astype(jnp.bfloat16)).astype(jnp.float32)
        summed = jnp.einsum('qhk,khe->qhe', rounded, values)
        return summed / total[..., None]

    def attend(block):
        first_q, second_q = block
        mixed = one_map(first_q, k_first) - mixing[None, :, None] * one_map(second_q, k_second)
        normed = mixed * lax.rsqrt(lax.optimization_barrier(jnp.mean(mixed * mixed, axis=-1, keepdims=True)) + epsilon) * head_gain
        return normed.astype(jnp.bfloat16)
    count = TOKENS // block_rows
    heads = lax.map(attend, (q_first.reshape(count, block_rows, HEADS, HEAD), q_second.reshape(count, block_rows, HEADS, HEAD)))
    heads = heads.reshape(TOKENS, HEADS * 2 * HEAD)
    return jnp.dot(heads, out_weight, preferred_element_type=jnp.float32).astype(jnp.bfloat16)
```

```python
import functools

import jax
import jax.numpy as jnp
import numpy as np
from jax import lax
from jax.experimental import pallas as pl
from jax.experimental.pallas import tpu as pltpu
from jax.sharding import PartitionSpec as P

HEAD = 64
GRID_W = 64
PAIR = 2 * HEAD

epsilon = 1e-06
theta_base = 10000.0
floor_value = -1e30
ring_limit = 16
chunk_rows = 1024
log2_e = 1.4426950408889634
MIB = 1 << 20
stage_grant = 52 * MIB

CONTRACT_LAST = (((1,), (1,)), ((), ()))


def turn_of(start, count):
    quarter = HEAD // 4
    lane = lax.broadcasted_iota(jnp.int32, (1, PAIR), 1)
    index = lane % quarter
    freqs = jnp.zeros((1, PAIR), jnp.float32)
    for j in range(quarter):
        freqs = jnp.where(index == j, theta_base ** (-j / quarter), freqs)
    token = start + lax.broadcasted_iota(jnp.int32, (count, PAIR), 0)
    by_row = (lane & (HEAD // 2)) == 0
    position = jnp.where(by_row, token // GRID_W, token % GRID_W).astype(jnp.float32)
    angle = position * freqs
    sine = jnp.sin(angle)
    return jnp.cos(angle), jnp.where((lane & quarter) == 0, -sine, sine)


def turned(field, cosine, sine):
    lane = lax.broadcasted_iota(jnp.int32, field.shape, 1)
    ahead = pltpu.roll(field, PAIR - HEAD // 4, 1)
    behind = pltpu.roll(field, HEAD // 4, 1)
    partner = jnp.where((lane & (HEAD // 4)) == 0, ahead, behind)
    return (field * cosine + partner * sine).astype(jnp.bfloat16)


def project_block(tokens, start, weight_refs, heads, q_ref, kv_ref, place):
    one_q, two_q, one_k, two_k, upper, lower = weight_refs
    count = tokens.shape[0]
    cosine, sine = turn_of(start, count)
    for head in range(heads):
        rows = slice(head * HEAD, (head + 1) * HEAD)

        def pair(first_w, second_w):
            return jnp.concatenate(
                [
                    lax.dot_general(
                        tokens, w[rows, :], CONTRACT_LAST, preferred_element_type=jnp.float32
                    )
                    for w in (first_w, second_w)
                ],
                axis=1,
            )

        columns = slice(head * PAIR, (head + 1) * PAIR)
        base = head * 2 * PAIR
        q_ref[place, columns] = turned(pair(one_q, two_q), cosine, sine)
        kv_ref[place, base : base + PAIR] = turned(pair(one_k, two_k), cosine, sine)
        half = upper.shape[0]
        values = jnp.dot(
            tokens[:, :half], upper[:, columns], preferred_element_type=jnp.float32
        ) + jnp.dot(tokens[:, half:], lower[:, columns], preferred_element_type=jnp.float32)
        kv_ref[place, base + PAIR : base + 2 * PAIR] = values.astype(jnp.bfloat16)


def start_of(step, count, groups):
    return (lax.axis_index("sp") * groups + (lax.axis_index("tp") ^ step)) * count


def stage_kernel(count, *refs):
    sources, held, sems = refs[:count], refs[count:-1], refs[-1]
    half = sources[-1].shape[0] // 2
    sources = [*sources[:-1], sources[-1].at[pl.ds(0, half)], sources[-1].at[pl.ds(half, half)]]
    copies = [pltpu.make_async_copy(a, b, sems.at[i]) for i, (a, b) in enumerate(zip(sources, held))]
    for copy in copies:
        copy.start()
    for copy in copies:
        copy.wait()


def shapes_of(rows, heads):
    return [
        jax.ShapeDtypeStruct((rows, heads * PAIR), jnp.bfloat16),
        jax.ShapeDtypeStruct((rows, heads * 2 * PAIR), jnp.bfloat16),
    ]


def project_cost(rows, depth, heads):
    return pl.CostEstimate(
        flops=2 * rows * depth * heads * 3 * PAIR, bytes_accessed=0, transcendentals=0
    )


def stage(arrays):
    size = sum(a.size * 2 for a in arrays)
    rows, columns = arrays[-1].shape
    shapes = [a.shape for a in arrays[:-1]] + [(rows // 2, columns)] * 2
    return pl.pallas_call(
        functools.partial(stage_kernel, len(arrays)),
        out_shape=[jax.ShapeDtypeStruct(shape, arrays[0].dtype) for shape in shapes],
        in_specs=[pl.BlockSpec(memory_space=pltpu.HBM)] * len(arrays),
        scratch_shapes=[pltpu.SemaphoreType.DMA((len(shapes),))],
        cost_estimate=pl.CostEstimate(flops=size * 256, bytes_accessed=size, transcendentals=0),
        compiler_params=pltpu.CompilerParams(vmem_limit_bytes=stage_grant),
        name="stage",
    )(*arrays)


def project_kernel(heads, groups, steps, *refs):
    blocks, refs = refs[: len(steps)], refs[len(steps) :]
    weight_refs, (q_ref, kv_ref) = refs[:6], refs[6:]
    count = blocks[0].shape[0]
    for at, (step, block) in enumerate(zip(steps, blocks)):
        project_block(
            block[...],
            start_of(step, count, groups),
            weight_refs,
            heads,
            q_ref,
            kv_ref,
            slice(at * count, (at + 1) * count),
        )


def project(blocks, steps, weights, heads, groups):
    count, depth = blocks[0].shape
    rows = count * len(blocks)
    return pl.pallas_call(
        functools.partial(project_kernel, heads, groups, steps),
        out_shape=shapes_of(rows, heads),
        cost_estimate=project_cost(rows, depth, heads),
        compiler_params=pltpu.CompilerParams(vmem_limit_bytes=8 * MIB),
        name="project",
    )(*blocks, *weights)


def finish_kernel(heads, groups, steps, last, *refs):
    earlier = refs[: 2 * len(steps)]
    block, *refs = refs[2 * len(steps) :]
    weight_refs, (q_ref, kv_ref) = refs[:6], refs[6:]
    count = block.shape[0]
    me = lax.axis_index("tp")
    for held, part_steps in enumerate(steps):
        for at, step in enumerate(part_steps):
            place = pl.ds(pl.multiple_of((me ^ step) * count, count), count)
            rows = slice(at * count, (at + 1) * count)
            q_ref[place, :] = earlier[2 * held][rows, :]
            kv_ref[place, :] = earlier[2 * held + 1][rows, :]
    project_block(
        block[...],
        start_of(last, count, groups),
        weight_refs,
        heads,
        q_ref,
        kv_ref,
        pl.ds(pl.multiple_of((me ^ last) * count, count), count),
    )


def finish(earlier, steps, block, last, weights, heads, groups):
    count, depth = block.shape
    return pl.pallas_call(
        functools.partial(finish_kernel, heads, groups, steps, last),
        out_shape=shapes_of(count * groups, heads),
        cost_estimate=project_cost(count, depth, heads),
        compiler_params=pltpu.CompilerParams(vmem_limit_bytes=8 * MIB),
        name="finish",
    )(*earlier, block, *weights)


def attend_kernel(heads, pieces, q_ref, *refs):
    kv_refs = refs[:pieces]
    mixing_ref, gain_ref = refs[pieces : pieces + 2]
    hold_ref = refs[-1]
    out_refs = refs[pieces + 2 : -1]
    rows = q_ref.shape[0]
    scale = HEAD ** (-0.5) * log2_e
    for head in range(heads):
        pair = q_ref[:, head * PAIR : (head + 1) * PAIR]
        lane = lax.broadcasted_iota(jnp.int32, pair.shape, 1)
        nothing = jnp.zeros_like(pair)
        both = jnp.concatenate(
            [jnp.where(lane < HEAD, pair, nothing), jnp.where(lane < HEAD, nothing, pair)], axis=0
        )
        base = head * 2 * PAIR

        def scores_of(ref, at, size):
            keys = ref[pl.ds(at, size), base : base + PAIR]
            return lax.dot_general(both, keys, CONTRACT_LAST, preferred_element_type=jnp.float32)

        def summed_of(weights, ref, at, size):
            values = ref[pl.ds(at, size), base + PAIR : base + 2 * PAIR]
            return jnp.dot(
                weights.astype(jnp.bfloat16), values, preferred_element_type=jnp.float32
            )

        if all(ref.shape[0] <= chunk_rows for ref in kv_refs):
            scores = [scores_of(ref, 0, ref.shape[0]) for ref in kv_refs]
            peak = functools.reduce(
                jnp.maximum, [jnp.max(s, axis=1, keepdims=True) for s in scores]
            )
            total = jnp.zeros((2 * rows, 1), jnp.float32)
            summed = jnp.zeros((2 * rows, PAIR), jnp.float32)
            for s, ref in zip(scores, kv_refs):
                weights = jnp.exp2((s - peak) * scale)
                total += jnp.sum(weights, axis=1, keepdims=True)
                summed += summed_of(weights, ref, 0, ref.shape[0])
        else:
            state = (
                jnp.full((2 * rows, 1), floor_value, jnp.float32),
                jnp.zeros((2 * rows, 1), jnp.float32),
                jnp.zeros((2 * rows, PAIR), jnp.float32),
            )
            for ref in kv_refs:
                size = np.gcd(ref.shape[0], chunk_rows).item()

                def step(index, carry, ref=ref, size=size):
                    peak, total, summed = carry
                    at = pl.multiple_of(index * size, size)
                    scores = scores_of(ref, at, size)
                    new_peak = jnp.maximum(peak, jnp.max(scores, axis=1, keepdims=True))
                    factor = jnp.exp2((peak - new_peak) * scale)
                    weights = jnp.exp2((scores - new_peak) * scale)
                    return (
                        new_peak,
                        total * factor + jnp.sum(weights, axis=1, keepdims=True),
                        summed * factor + summed_of(weights, ref, at, size),
                    )

                state = lax.fori_loop(0, ref.shape[0] // size, step, state)
            total, summed = state[1:]
        ratio = summed / total
        mixed = ratio[:rows] - mixing_ref[head] * ratio[rows:]
        square = jnp.mean(mixed * mixed, axis=1, keepdims=True)
        normed = mixed * lax.rsqrt(square + epsilon) * gain_ref[...]
        hold_ref[...] = normed
        me = lax.axis_index("tp")
        share = rows // len(out_refs)
        for step, out_ref in enumerate(out_refs):
            at = pl.multiple_of((me ^ step) * share, share)
            out_ref[:, head * PAIR : (head + 1) * PAIR] = hold_ref[pl.ds(at, share), :].astype(
                jnp.bfloat16
            )


def attend_grant(rows, keys, heads):
    held = 4 * rows * min(keys, chunk_rows) * 8 + 2 * keys * heads * 2 * PAIR
    return held + 8 * MIB


def attend(queries, pieces, mixing, gain, heads, groups):
    rows = queries.shape[0]
    keys = sum(p.shape[0] for p in pieces)
    vmem = pl.BlockSpec(memory_space=pltpu.VMEM)
    return pl.pallas_call(
        functools.partial(attend_kernel, heads, len(pieces)),
        out_shape=[jax.ShapeDtypeStruct((rows // groups, heads * PAIR), jnp.bfloat16)] * groups,
        scratch_shapes=[pltpu.VMEM((rows, PAIR), jnp.float32)],
        in_specs=[vmem] * (1 + len(pieces)) + [pl.BlockSpec(memory_space=pltpu.SMEM), vmem],
        cost_estimate=pl.CostEstimate(
            flops=2 * 4 * rows * keys * heads * PAIR,
            bytes_accessed=2 * keys * heads * 2 * PAIR,
            transcendentals=2 * rows * keys * heads,
        ),
        compiler_params=pltpu.CompilerParams(vmem_limit_bytes=attend_grant(rows, keys, heads)),
        name="attend",
    )(queries, *pieces, mixing, gain.reshape(1, PAIR))


def output_kernel(count, *refs):
    piece_refs = refs[:count]
    weight_ref, out_ref = refs[count:]
    width = piece_refs[0].shape[1]
    me = lax.axis_index("tp")
    total = None
    for step in range(count):
        at = pl.multiple_of((me ^ step) * width, width)
        part = jnp.dot(
            piece_refs[step][...], weight_ref[pl.ds(at, width), :], preferred_element_type=jnp.float32
        )
        total = part if total is None else total + part
    out_ref[...] = total.astype(jnp.bfloat16)


def output(pieces, weight):
    rows, width = pieces[0].shape
    return pl.pallas_call(
        functools.partial(output_kernel, len(pieces)),
        out_shape=jax.ShapeDtypeStruct((rows, weight.shape[1]), jnp.bfloat16),
        cost_estimate=pl.CostEstimate(
            flops=2 * rows * weight.shape[0] * weight.shape[1],
            bytes_accessed=2 * weight.size,
            transcendentals=0,
        ),
        compiler_params=pltpu.CompilerParams(vmem_limit_bytes=8 * MIB),
        name="output",
    )(*pieces, weight)


def exchange(block, axis, step):
    size = lax.axis_size(axis)
    return lax.ppermute(block, axis, [(i, i ^ step) for i in range(size)])


def gather_pieces(packed, axis):
    size = lax.axis_size(axis)
    if size > ring_limit or size & (size - 1):
        return [lax.all_gather(packed, axis, axis=0, tiled=True)]
    half = size // 2
    far = exchange(packed, axis, half)
    near = [exchange(packed, axis, step) for step in range(1, half)]
    forwarded = [exchange(far, axis, step) for step in range(1, half)]
    return [packed, far] + near + forwarded


def per_device(
    tokens, query_one, query_two, key_one, key_two, value_weight, mixing, out_weight, head_gain
):
    groups = lax.axis_size("tp")
    own_rows = tokens.shape[0]
    row_count = own_rows * groups
    heads = query_one.shape[1] // HEAD
    weights = (query_one.T, query_two.T, key_one.T, key_two.T, value_weight)
    across = exchange(tokens, "tp", 2)
    beside = exchange(tokens, "tp", 1)
    own, *held = stage([tokens, *weights])
    across, own = lax.optimization_barrier((across, own))
    last = exchange(across, "tp", 1)
    early = project([own, beside, across], (0, 1, 2), held, heads, groups)
    queries, packed = finish(early, ((0, 1, 2),), last, 3, held, heads, groups)
    pieces = gather_pieces(packed, "sp")
    shares = attend(queries, pieces, mixing, head_gain, heads, groups)
    parts = [exchange(share, "tp", step) if step else share for step, share in enumerate(shares)]
    return output(parts, out_weight)


def solution(mesh):
    in_specs = (
        P(("sp", "tp"), None),
        P(None, "tp"),
        P(None, "tp"),
        P(None, "tp"),
        P(None, "tp"),
        P(None, "tp"),
        P("tp"),
        P(),
        P(),
    )
    out_specs = P(("sp", "tp"), None)
    return jax.shard_map(
        per_device, mesh=mesh, in_specs=in_specs, out_specs=out_specs, check_vma=False
    )
```

```python
import functools

import jax
import jax.numpy as jnp
import numpy as np
from jax import lax
from jax.experimental import pallas as pl
from jax.experimental.pallas import tpu as pltpu
from jax.sharding import PartitionSpec as P

HEAD = 64
GRID_W = 64
PAIR = 2 * HEAD

epsilon = 1e-06
theta_base = 10000.0
floor_value = -1e30
ring_limit = 16
chunk_rows = 1024
log2_e = 1.4426950408889634
MIB = 1 << 20
stage_grant = 52 * MIB

CONTRACT_LAST = (((1,), (1,)), ((), ()))


def turn_of(start, count):
    quarter = HEAD // 4
    lane = lax.broadcasted_iota(jnp.int32, (1, PAIR), 1)
    index = lane % quarter
    freqs = jnp.zeros((1, PAIR), jnp.float32)
    for j in range(quarter):
        freqs = jnp.where(index == j, theta_base ** (-j / quarter), freqs)
    token = start + lax.broadcasted_iota(jnp.int32, (count, PAIR), 0)
    by_row = (lane & (HEAD // 2)) == 0
    position = jnp.where(by_row, token // GRID_W, token % GRID_W).astype(jnp.float32)
    angle = position * freqs
    sine = jnp.sin(angle)
    return jnp.cos(angle), jnp.where((lane & quarter) == 0, -sine, sine)


def turned(field, cosine, sine):
    lane = lax.broadcasted_iota(jnp.int32, field.shape, 1)
    ahead = pltpu.roll(field, PAIR - HEAD // 4, 1)
    behind = pltpu.roll(field, HEAD // 4, 1)
    partner = jnp.where((lane & (HEAD // 4)) == 0, ahead, behind)
    return (field * cosine + partner * sine).astype(jnp.bfloat16)


def project_blocks(blocks, places, weight_refs, heads, q_ref, kv_ref, place):
    one_q, two_q, one_k, two_k, upper, lower, cosine_ref, sine_ref = weight_refs
    count = blocks[0].shape[0]
    tokens = jnp.concatenate([block[...] for block in blocks], axis=0)
    cosine, sine = [
        jnp.concatenate([ref[pl.ds(at, count), :] for at in places], axis=0)
        for ref in (cosine_ref, sine_ref)
    ]
    half = upper.shape[0]
    for head in range(heads):
        rows = slice(head * HEAD, (head + 1) * HEAD)
        columns = slice(head * PAIR, (head + 1) * PAIR)
        base = head * 2 * PAIR

        def turned_pair(first, second):
            joined = jnp.concatenate([first[rows, :], second[rows, :]], axis=0)
            pair = lax.dot_general(
                tokens, joined, CONTRACT_LAST, preferred_element_type=jnp.float32
            )
            return turned(pair, cosine, sine)

        if kv_ref is not None:
            kv_ref[place, base : base + PAIR] = turned_pair(one_k, two_k)
            values = jnp.dot(
                tokens[:, :half], upper[:, columns], preferred_element_type=jnp.float32
            ) + jnp.dot(tokens[:, half:], lower[:, columns], preferred_element_type=jnp.float32)
            kv_ref[place, base + PAIR : base + 2 * PAIR] = values.astype(jnp.bfloat16)
        if q_ref is not None:
            q_ref[place, columns] = turned_pair(one_q, two_q)


def place_of(step, count):
    return pl.multiple_of((lax.axis_index("tp") ^ step) * count, count)


def stage_kernel(count, *refs):
    sources, held, (cosine_ref, sine_ref, sems) = refs[:count], refs[count:-3], refs[-3:]
    half = sources[-1].shape[0] // 2
    sources = [*sources[:-1], sources[-1].at[pl.ds(0, half)], sources[-1].at[pl.ds(half, half)]]
    copies = [pltpu.make_async_copy(a, b, sems.at[i]) for i, (a, b) in enumerate(zip(sources, held))]
    for copy in copies:
        copy.start()
    rows = cosine_ref.shape[0]
    cosine_ref[...], sine_ref[...] = turn_of(lax.axis_index("sp") * rows, rows)
    for copy in copies:
        copy.wait()


def shapes_of(rows, heads):
    return [
        jax.ShapeDtypeStruct((rows, heads * PAIR), jnp.bfloat16),
        jax.ShapeDtypeStruct((rows, heads * 2 * PAIR), jnp.bfloat16),
    ]


def project_cost(rows, depth, heads):
    return pl.CostEstimate(
        flops=2 * rows * depth * heads * 3 * PAIR, bytes_accessed=0, transcendentals=0
    )


def stage(arrays, total):
    size = sum(a.size * 2 for a in arrays)
    rows, columns = arrays[-1].shape
    shapes = [a.shape for a in arrays[:-1]] + [(rows // 2, columns)] * 2
    return pl.pallas_call(
        functools.partial(stage_kernel, len(arrays)),
        out_shape=[jax.ShapeDtypeStruct(shape, arrays[0].dtype) for shape in shapes]
        + [jax.ShapeDtypeStruct((total, PAIR), jnp.float32)] * 2,
        in_specs=[pl.BlockSpec(memory_space=pltpu.HBM)] * len(arrays),
        scratch_shapes=[pltpu.SemaphoreType.DMA((len(shapes),))],
        cost_estimate=pl.CostEstimate(flops=size * 256, bytes_accessed=size, transcendentals=0),
        compiler_params=pltpu.CompilerParams(vmem_limit_bytes=stage_grant),
        name="stage",
    )(*arrays)


def project_kernel(heads, steps, *refs):
    blocks, refs = refs[: len(steps)], refs[len(steps) :]
    weight_refs, (q_ref, kv_ref) = refs[:8], refs[8:]
    places = [place_of(step, blocks[0].shape[0]) for step in steps]
    project_blocks(blocks, places, weight_refs, heads, q_ref, kv_ref, slice(None))


def project(blocks, steps, weights, heads):
    count, depth = blocks[0].shape
    rows = count * len(blocks)
    return pl.pallas_call(
        functools.partial(project_kernel, heads, steps),
        out_shape=shapes_of(rows, heads),
        cost_estimate=project_cost(rows, depth, heads),
        compiler_params=pltpu.CompilerParams(vmem_limit_bytes=8 * MIB),
        name="project",
    )(*blocks, *weights)


def finish_kernel(heads, steps, last, keys, early_ref, block_ref, *refs):
    weight_refs, out_ref = refs[:8], refs[8]
    count = block_ref.shape[0]
    for at, step in enumerate(steps):
        out_ref[pl.ds(place_of(step, count), count), :] = early_ref[at * count : (at + 1) * count, :]
    place = place_of(last, count)
    project_blocks(
        [block_ref],
        [place],
        weight_refs,
        heads,
        None if keys else out_ref,
        out_ref if keys else None,
        pl.ds(place, count),
    )


def finish(early, steps, block, last, weights, heads, groups, keys):
    count, depth = block.shape
    return pl.pallas_call(
        functools.partial(finish_kernel, heads, steps, last, keys),
        out_shape=jax.ShapeDtypeStruct((count * groups, early.shape[1]), early.dtype),
        cost_estimate=project_cost(count, depth, heads),
        compiler_params=pltpu.CompilerParams(vmem_limit_bytes=8 * MIB),
        name="keys" if keys else "queries",
    )(early, block, *weights)


def both_of(pair):
    lane = lax.broadcasted_iota(jnp.int32, pair.shape, 1)
    nothing = jnp.zeros_like(pair)
    return jnp.concatenate(
        [jnp.where(lane < HEAD, pair, nothing), jnp.where(lane < HEAD, nothing, pair)], axis=0
    )


def absorb(state, both, kv_refs, head):
    scale = HEAD ** (-0.5) * log2_e
    base = head * 2 * PAIR

    def taken(carry, parts):
        scores = [
            lax.dot_general(
                both,
                ref[rows, base : base + PAIR],
                CONTRACT_LAST,
                preferred_element_type=jnp.float32,
            )
            for ref, rows in parts
        ]
        peaks = [jnp.max(s, axis=1, keepdims=True) for s in scores]
        if carry is None:
            peak, total, summed = functools.reduce(jnp.maximum, peaks), None, None
        else:
            before, total, summed = carry
            peak = functools.reduce(jnp.maximum, peaks, before)
            factor = jnp.exp2((before - peak) * scale)
            total, summed = total * factor, summed * factor
        for s, (ref, rows) in zip(scores, parts):
            weights = jnp.exp2((s - peak) * scale)
            partial = jnp.sum(weights, axis=1, keepdims=True)
            product = jnp.dot(
                weights.astype(jnp.bfloat16),
                ref[rows, base + PAIR : base + 2 * PAIR],
                preferred_element_type=jnp.float32,
            )
            total = partial if total is None else total + partial
            summed = product if summed is None else summed + product
        return peak, total, summed

    if sum(ref.shape[0] for ref in kv_refs) <= chunk_rows:
        return taken(state, [(ref, slice(None)) for ref in kv_refs])
    for ref in kv_refs:
        size = np.gcd(ref.shape[0], chunk_rows).item()
        if state is None:
            rows = both.shape[0]
            state = (
                jnp.full((rows, 1), floor_value, jnp.float32),
                jnp.zeros((rows, 1), jnp.float32),
                jnp.zeros((rows, PAIR), jnp.float32),
            )

        def step(index, carry, ref=ref, size=size):
            return taken(carry, [(ref, pl.ds(pl.multiple_of(index * size, size), size))])

        state = lax.fori_loop(0, ref.shape[0] // size, step, state)
    return state


def begin_kernel(heads, pieces, held, q_ref, *refs):
    state_refs, kv_refs, out_refs = refs[:held], refs[held : held + pieces], refs[held + pieces :]
    for head in range(heads):
        state = tuple(ref[head] for ref in state_refs) or None
        both = both_of(q_ref[:, head * PAIR : (head + 1) * PAIR])
        for ref, value in zip(out_refs, absorb(state, both, kv_refs, head)):
            ref[head] = value


def attend_kernel(heads, pieces, held, groups, steps, q_ref, *refs):
    state_refs, refs = refs[:held], refs[held:]
    kv_refs, (mixing_ref, gain_ref), out_refs = refs[:pieces], refs[pieces : pieces + 2], refs[pieces + 2 :]
    total_rows = q_ref.shape[0]
    share = total_rows // groups
    rows = share * len(steps)
    places = [place_of(step, share) for step in steps]
    for head in range(heads):
        columns = slice(head * PAIR, (head + 1) * PAIR)
        pair = jnp.concatenate([q_ref[pl.ds(at, share), columns] for at in places], axis=0)
        state = None
        if held:
            spots = places + [total_rows + at for at in places]
            state = tuple(
                jnp.concatenate([ref[head, pl.ds(at, share), :] for at in spots], axis=0)
                for ref in state_refs
            )
        _, total, summed = absorb(state, both_of(pair), kv_refs, head)
        ratio = summed / total
        mixed = ratio[:rows] - mixing_ref[:, head : head + 1] * ratio[rows:]
        square = jnp.mean(mixed * mixed, axis=1, keepdims=True)
        normed = (mixed * lax.rsqrt(square + epsilon) * gain_ref[...]).astype(jnp.bfloat16)
        for at, out_ref in enumerate(out_refs):
            out_ref[:, columns] = normed[at * share : (at + 1) * share]


def attend_grant(rows, keys, heads):
    return 4 * rows * min(keys, chunk_rows) * 8 + 2 * keys * heads * 2 * PAIR + 8 * MIB


def attend_cost(rows, keys, heads):
    return pl.CostEstimate(
        flops=2 * 4 * rows * keys * heads * PAIR,
        bytes_accessed=0,
        transcendentals=2 * rows * keys * heads,
    )


def begin(queries, state, pieces, heads):
    rows = queries.shape[0]
    keys = sum(p.shape[0] for p in pieces)
    return pl.pallas_call(
        functools.partial(begin_kernel, heads, len(pieces), len(state)),
        out_shape=[
            jax.ShapeDtypeStruct((heads, 2 * rows, width), jnp.float32) for width in (1, 1, PAIR)
        ],
        cost_estimate=attend_cost(rows, keys, heads),
        compiler_params=pltpu.CompilerParams(vmem_limit_bytes=attend_grant(rows, keys, heads)),
        name="middle" if state else "begin",
    )(queries, *state, *pieces)


def attend(queries, state, pieces, mixing, gain, heads, groups, steps):
    rows = queries.shape[0]
    keys = sum(p.shape[0] for p in pieces)
    share = jax.ShapeDtypeStruct((rows // groups, heads * PAIR), jnp.bfloat16)
    return pl.pallas_call(
        functools.partial(attend_kernel, heads, len(pieces), len(state), groups, steps),
        out_shape=[share] * len(steps),
        cost_estimate=attend_cost(rows * len(steps) // groups, keys, heads),
        compiler_params=pltpu.CompilerParams(vmem_limit_bytes=attend_grant(rows, keys, heads)),
        name="attend",
    )(queries, *state, *pieces, mixing.reshape(1, heads), gain.reshape(1, PAIR))


def summed_shares(share_refs, steps, weight_ref, total):
    width = share_refs[0].shape[1]
    for step, ref in zip(steps, share_refs):
        part = jnp.dot(
            ref[...],
            weight_ref[pl.ds(place_of(step, width), width), :],
            preferred_element_type=jnp.float32,
        )
        total = part if total is None else total + part
    return total


def output_kernel(steps, held, *refs):
    share_refs, weight_ref, out_ref = refs[held : held + len(steps)], refs[-2], refs[-1]
    total = summed_shares(share_refs, steps, weight_ref, refs[0][...] if held else None)
    out_ref[...] = total.astype(out_ref.dtype)


def output(earlier, shares, steps, weight, dtype):
    rows, width = shares[0].shape
    return pl.pallas_call(
        functools.partial(output_kernel, steps, len(earlier)),
        out_shape=jax.ShapeDtypeStruct((rows, weight.shape[1]), dtype),
        cost_estimate=pl.CostEstimate(
            flops=2 * rows * width * len(steps) * weight.shape[1],
            bytes_accessed=0,
            transcendentals=0,
        ),
        compiler_params=pltpu.CompilerParams(vmem_limit_bytes=8 * MIB),
        name="output" if earlier else "early",
    )(*earlier, *shares, weight)


def exchange(block, axis, step):
    size = lax.axis_size(axis)
    return lax.ppermute(block, axis, [(i, i ^ step) for i in range(size)])


def gather_pieces(packed, axis):
    size = lax.axis_size(axis)
    if size > ring_limit or size & (size - 1):
        return [], [lax.all_gather(packed, axis, axis=0, tiled=True)]
    half = size // 2
    far = exchange(packed, axis, half)
    near = [exchange(packed, axis, step) for step in range(half - 1, 0, -1)]
    forwarded = [exchange(far, axis, step) for step in range(half - 1, 0, -1)]
    return [packed, far] + near, forwarded


def per_device(
    tokens, query_one, query_two, key_one, key_two, value_weight, mixing, out_weight, head_gain
):
    groups = lax.axis_size("tp")
    own_rows = tokens.shape[0]
    row_count = own_rows * groups
    heads = query_one.shape[1] // HEAD
    weights = (query_one.T, query_two.T, key_one.T, key_two.T, value_weight)
    across = exchange(tokens, "tp", 2)
    beside = exchange(tokens, "tp", 1)
    own, *held = stage([tokens, *weights], own_rows * groups)
    across, own = lax.optimization_barrier((across, own))
    last = exchange(across, "tp", 1)
    early = project([own, beside, across], (0, 1, 2), held, heads)
    packed = finish(early[1], (0, 1, 2), last, 3, held, heads, groups, True)
    queries = finish(early[0], (0, 1, 2), last, 3, held, heads, groups, False)
    first, second = gather_pieces(packed, "sp")
    state = begin(queries, [], first, heads) if first else []
    if len(second) > 1:
        state, second = begin(queries, state, second[:-1], heads), second[-1:]
    rest = (mixing, head_gain, heads, groups)
    own, beside, across, aside = attend(queries, state, second, *rest, (0, 1, 2, 3))
    across, aside = exchange(across, "tp", 2), exchange(aside, "tp", 3)
    beside = exchange(beside, "tp", 1)
    early = output([], [own, aside], (0, 3), out_weight, jnp.float32)
    return output([early], [across, beside], (2, 1), out_weight, jnp.bfloat16)


def solution(mesh):
    in_specs = (
        P(("sp", "tp"), None),
        P(None, "tp"),
        P(None, "tp"),
        P(None, "tp"),
        P(None, "tp"),
        P(None, "tp"),
        P("tp"),
        P(),
        P(),
    )
    out_specs = P(("sp", "tp"), None)
    return jax.shard_map(
        per_device, mesh=mesh, in_specs=in_specs, out_specs=out_specs, check_vma=False
    )
```

```python
import functools

import jax
import jax.numpy as jnp
import numpy as np
from jax import lax
from jax.experimental import pallas as pl
from jax.experimental.pallas import tpu as pltpu
from jax.sharding import PartitionSpec as P

HEAD = 64
GRID_W = 64
PAIR = 2 * HEAD

epsilon = 1e-06
theta_base = 10000.0
floor_value = -1e30
ring_limit = 16
chunk_rows = 1024
log2_e = 1.4426950408889634
MIB = 1 << 20
stage_grant = 52 * MIB

CONTRACT_LAST = (((1,), (1,)), ((), ()))


def turn_of(start, count):
    quarter = HEAD // 4
    lane = lax.broadcasted_iota(jnp.int32, (1, PAIR), 1)
    index = lane % quarter
    freqs = jnp.zeros((1, PAIR), jnp.float32)
    for j in range(quarter):
        freqs = jnp.where(index == j, theta_base ** (-j / quarter), freqs)
    token = start + lax.broadcasted_iota(jnp.int32, (count, PAIR), 0)
    by_row = (lane & (HEAD // 2)) == 0
    position = jnp.where(by_row, token // GRID_W, token % GRID_W).astype(jnp.float32)
    angle = position * freqs
    sine = jnp.sin(angle)
    return jnp.cos(angle), jnp.where((lane & quarter) == 0, -sine, sine)


def turned(field, cosine, sine):
    lane = lax.broadcasted_iota(jnp.int32, field.shape, 1)
    ahead = pltpu.roll(field, PAIR - HEAD // 4, 1)
    behind = pltpu.roll(field, HEAD // 4, 1)
    partner = jnp.where((lane & (HEAD // 4)) == 0, ahead, behind)
    return (field * cosine + partner * sine).astype(jnp.bfloat16)


def project_blocks(blocks, places, weight_refs, heads, q_ref, kv_ref, place):
    one_q, two_q, one_k, two_k, upper, lower, cosine_ref, sine_ref = weight_refs
    count = blocks[0].shape[0]
    tokens = jnp.concatenate([block[...] for block in blocks], axis=0)
    cosine, sine = [
        jnp.concatenate([ref[pl.ds(at, count), :] for at in places], axis=0)
        for ref in (cosine_ref, sine_ref)
    ]
    half = upper.shape[0]
    for head in range(heads):
        rows = slice(head * HEAD, (head + 1) * HEAD)
        columns = slice(head * PAIR, (head + 1) * PAIR)
        base = head * 2 * PAIR

        def turned_pair(first, second):
            joined = jnp.concatenate([first[rows, :], second[rows, :]], axis=0)
            pair = lax.dot_general(
                tokens, joined, CONTRACT_LAST, preferred_element_type=jnp.float32
            )
            return turned(pair, cosine, sine)

        if kv_ref is not None:
            kv_ref[place, base : base + PAIR] = turned_pair(one_k, two_k)
            values = jnp.dot(
                tokens[:, :half], upper[:, columns], preferred_element_type=jnp.float32
            ) + jnp.dot(tokens[:, half:], lower[:, columns], preferred_element_type=jnp.float32)
            kv_ref[place, base + PAIR : base + 2 * PAIR] = values.astype(jnp.bfloat16)
        if q_ref is not None:
            q_ref[place, columns] = turned_pair(one_q, two_q)


def place_of(step, count):
    return pl.multiple_of((lax.axis_index("tp") ^ step) * count, count)


def stage_kernel(count, *refs):
    sources, held, (cosine_ref, sine_ref, sems) = refs[:count], refs[count:-3], refs[-3:]
    half = sources[-1].shape[0] // 2
    sources = [*sources[:-1], sources[-1].at[pl.ds(0, half)], sources[-1].at[pl.ds(half, half)]]
    copies = [pltpu.make_async_copy(a, b, sems.at[i]) for i, (a, b) in enumerate(zip(sources, held))]
    for copy in copies:
        copy.start()
    rows = cosine_ref.shape[0]
    cosine_ref[...], sine_ref[...] = turn_of(lax.axis_index("sp") * rows, rows)
    for copy in copies:
        copy.wait()


def shapes_of(rows, heads):
    return [
        jax.ShapeDtypeStruct((rows, heads * PAIR), jnp.bfloat16),
        jax.ShapeDtypeStruct((rows, heads * 2 * PAIR), jnp.bfloat16),
    ]


def project_cost(rows, depth, heads):
    return pl.CostEstimate(
        flops=2 * rows * depth * heads * 3 * PAIR, bytes_accessed=0, transcendentals=0
    )


def stage(arrays, total):
    size = sum(a.size * 2 for a in arrays)
    rows, columns = arrays[-1].shape
    shapes = [a.shape for a in arrays[:-1]] + [(rows // 2, columns)] * 2
    return pl.pallas_call(
        functools.partial(stage_kernel, len(arrays)),
        out_shape=[jax.ShapeDtypeStruct(shape, arrays[0].dtype) for shape in shapes]
        + [jax.ShapeDtypeStruct((total, PAIR), jnp.float32)] * 2,
        in_specs=[pl.BlockSpec(memory_space=pltpu.HBM)] * len(arrays),
        scratch_shapes=[pltpu.SemaphoreType.DMA((len(shapes),))],
        cost_estimate=pl.CostEstimate(flops=size * 256, bytes_accessed=size, transcendentals=0),
        compiler_params=pltpu.CompilerParams(vmem_limit_bytes=stage_grant),
        name="stage",
    )(*arrays)


def project_kernel(heads, steps, *refs):
    blocks, refs = refs[: len(steps)], refs[len(steps) :]
    weight_refs, (q_ref, kv_ref) = refs[:8], refs[8:]
    places = [place_of(step, blocks[0].shape[0]) for step in steps]
    project_blocks(blocks, places, weight_refs, heads, q_ref, kv_ref, slice(None))


def project(blocks, steps, weights, heads):
    count, depth = blocks[0].shape
    rows = count * len(blocks)
    return pl.pallas_call(
        functools.partial(project_kernel, heads, steps),
        out_shape=shapes_of(rows, heads),
        cost_estimate=project_cost(rows, depth, heads),
        compiler_params=pltpu.CompilerParams(vmem_limit_bytes=8 * MIB),
        name="project",
    )(*blocks, *weights)


def finish_kernel(heads, steps, late_steps, keys, early_ref, *refs):
    blocks, refs = refs[: len(late_steps)], refs[len(late_steps) :]
    weight_refs, out_ref = refs[:8], refs[8]
    count = blocks[0].shape[0]
    for at, step in enumerate(steps):
        out_ref[pl.ds(place_of(step, count), count), :] = early_ref[at * count : (at + 1) * count, :]
    for step, block in zip(late_steps, blocks):
        place = place_of(step, count)
        project_blocks(
            [block],
            [place],
            weight_refs,
            heads,
            None if keys else out_ref,
            out_ref if keys else None,
            pl.ds(place, count),
        )


def finish(early, steps, blocks, late_steps, weights, heads, groups, keys):
    count, depth = blocks[0].shape
    return pl.pallas_call(
        functools.partial(finish_kernel, heads, steps, late_steps, keys),
        out_shape=jax.ShapeDtypeStruct((count * groups, early.shape[1]), early.dtype),
        cost_estimate=project_cost(count * len(blocks), depth, heads),
        compiler_params=pltpu.CompilerParams(vmem_limit_bytes=8 * MIB),
        name="keys" if keys else "queries",
    )(early, *blocks, *weights)


def both_of(pair):
    lane = lax.broadcasted_iota(jnp.int32, pair.shape, 1)
    nothing = jnp.zeros_like(pair)
    return jnp.concatenate(
        [jnp.where(lane < HEAD, pair, nothing), jnp.where(lane < HEAD, nothing, pair)], axis=0
    )


def absorb(state, both, kv_refs, head):
    scale = HEAD ** (-0.5) * log2_e
    base = head * 2 * PAIR

    def taken(carry, parts):
        scores = [
            lax.dot_general(
                both,
                ref[rows, base : base + PAIR],
                CONTRACT_LAST,
                preferred_element_type=jnp.float32,
            )
            for ref, rows in parts
        ]
        peaks = [jnp.max(s, axis=1, keepdims=True) for s in scores]
        if carry is None:
            peak, total, summed = functools.reduce(jnp.maximum, peaks), None, None
        else:
            before, total, summed = carry
            peak = functools.reduce(jnp.maximum, peaks, before)
            factor = jnp.exp2((before - peak) * scale)
            total, summed = total * factor, summed * factor
        for s, (ref, rows) in zip(scores, parts):
            weights = jnp.exp2((s - peak) * scale)
            partial = jnp.sum(weights, axis=1, keepdims=True)
            product = jnp.dot(
                weights.astype(jnp.bfloat16),
                ref[rows, base + PAIR : base + 2 * PAIR],
                preferred_element_type=jnp.float32,
            )
            total = partial if total is None else total + partial
            summed = product if summed is None else summed + product
        return peak, total, summed

    if sum(ref.shape[0] for ref in kv_refs) <= chunk_rows:
        return taken(state, [(ref, slice(None)) for ref in kv_refs])
    for ref in kv_refs:
        size = np.gcd(ref.shape[0], chunk_rows).item()
        if state is None:
            rows = both.shape[0]
            state = (
                jnp.full((rows, 1), floor_value, jnp.float32),
                jnp.zeros((rows, 1), jnp.float32),
                jnp.zeros((rows, PAIR), jnp.float32),
            )

        def step(index, carry, ref=ref, size=size):
            return taken(carry, [(ref, pl.ds(pl.multiple_of(index * size, size), size))])

        state = lax.fori_loop(0, ref.shape[0] // size, step, state)
    return state


def begin_kernel(heads, pieces, held, q_ref, *refs):
    state_refs, kv_refs, out_refs = refs[:held], refs[held : held + pieces], refs[held + pieces :]
    for head in range(heads):
        state = tuple(ref[head] for ref in state_refs) or None
        both = both_of(q_ref[:, head * PAIR : (head + 1) * PAIR])
        for ref, value in zip(out_refs, absorb(state, both, kv_refs, head)):
            ref[head] = value


def attend_kernel(heads, pieces, held, groups, q_ref, *refs):
    state_refs, refs = refs[:held], refs[held:]
    kv_refs, (mixing_ref, gain_ref), out_refs = refs[:pieces], refs[pieces : pieces + 2], refs[pieces + 2 :]
    total_rows = q_ref.shape[0]
    share = total_rows // groups
    rows = total_rows
    places = [place_of(step, share) for step in range(groups)]
    for head in range(heads):
        columns = slice(head * PAIR, (head + 1) * PAIR)
        pair = jnp.concatenate([q_ref[pl.ds(at, share), columns] for at in places], axis=0)
        state = None
        if held:
            spots = places + [total_rows + at for at in places]
            state = tuple(
                jnp.concatenate([ref[head, pl.ds(at, share), :] for at in spots], axis=0)
                for ref in state_refs
            )
        _, total, summed = absorb(state, both_of(pair), kv_refs, head)
        ratio = summed / total
        mixed = ratio[:rows] - mixing_ref[:, head : head + 1] * ratio[rows:]
        square = jnp.mean(mixed * mixed, axis=1, keepdims=True)
        normed = (mixed * lax.rsqrt(square + epsilon) * gain_ref[...]).astype(jnp.bfloat16)
        for at, out_ref in enumerate(out_refs):
            out_ref[:, columns] = normed[at * share : (at + 1) * share]


def attend_grant(rows, keys, heads):
    return 4 * rows * min(keys, chunk_rows) * 8 + 2 * keys * heads * 2 * PAIR + 8 * MIB


def attend_cost(rows, keys, heads):
    return pl.CostEstimate(
        flops=2 * 4 * rows * keys * heads * PAIR,
        bytes_accessed=0,
        transcendentals=2 * rows * keys * heads,
    )


def begin(queries, state, pieces, heads):
    rows = queries.shape[0]
    keys = sum(p.shape[0] for p in pieces)
    return pl.pallas_call(
        functools.partial(begin_kernel, heads, len(pieces), len(state)),
        out_shape=[
            jax.ShapeDtypeStruct((heads, 2 * rows, width), jnp.float32) for width in (1, 1, PAIR)
        ],
        cost_estimate=attend_cost(rows, keys, heads),
        compiler_params=pltpu.CompilerParams(vmem_limit_bytes=attend_grant(rows, keys, heads)),
        name="middle" if state else "begin",
    )(queries, *state, *pieces)


def attend(queries, state, pieces, mixing, gain, heads, groups):
    rows = queries.shape[0]
    keys = sum(p.shape[0] for p in pieces)
    share = jax.ShapeDtypeStruct((rows // groups, heads * PAIR), jnp.bfloat16)
    return pl.pallas_call(
        functools.partial(attend_kernel, heads, len(pieces), len(state), groups),
        out_shape=[share] * groups,
        cost_estimate=attend_cost(rows, keys, heads),
        compiler_params=pltpu.CompilerParams(vmem_limit_bytes=attend_grant(rows, keys, heads)),
        name="attend",
    )(queries, *state, *pieces, mixing.reshape(1, heads), gain.reshape(1, PAIR))


def summed_shares(share_refs, steps, weight_ref, total):
    width = share_refs[0].shape[1]
    for step, ref in zip(steps, share_refs):
        part = jnp.dot(
            ref[...],
            weight_ref[pl.ds(place_of(step, width), width), :],
            preferred_element_type=jnp.float32,
        )
        total = part if total is None else total + part
    return total


def output_kernel(steps, held, *refs):
    share_refs, weight_ref, out_ref = refs[held : held + len(steps)], refs[-2], refs[-1]
    total = summed_shares(share_refs, steps, weight_ref, refs[0][...] if held else None)
    out_ref[...] = total.astype(out_ref.dtype)


def output(earlier, shares, steps, weight, dtype):
    rows, width = shares[0].shape
    return pl.pallas_call(
        functools.partial(output_kernel, steps, len(earlier)),
        out_shape=jax.ShapeDtypeStruct((rows, weight.shape[1]), dtype),
        cost_estimate=pl.CostEstimate(
            flops=2 * rows * width * len(steps) * weight.shape[1],
            bytes_accessed=0,
            transcendentals=0,
        ),
        compiler_params=pltpu.CompilerParams(vmem_limit_bytes=8 * MIB),
        name="output" if earlier else "early",
    )(*earlier, *shares, weight)


def exchange(block, axis, step):
    size = lax.axis_size(axis)
    return lax.ppermute(block, axis, [(i, i ^ step) for i in range(size)])


def gather_pieces(packed, axis):
    size = lax.axis_size(axis)
    if size > ring_limit or size & (size - 1):
        return [], [lax.all_gather(packed, axis, axis=0, tiled=True)]
    half = size // 2
    far = exchange(packed, axis, half)
    near = [exchange(packed, axis, step) for step in range(half - 1, 0, -1)]
    forwarded = [exchange(far, axis, step) for step in range(half - 1, 0, -1)]
    return [packed, far] + near, forwarded


def per_device(
    tokens, query_one, query_two, key_one, key_two, value_weight, mixing, out_weight, head_gain
):
    groups = lax.axis_size("tp")
    own_rows = tokens.shape[0]
    row_count = own_rows * groups
    heads = query_one.shape[1] // HEAD
    weights = (query_one.T, query_two.T, key_one.T, key_two.T, value_weight)
    half = groups // 2
    near = tuple(range(1, half))
    across = exchange(tokens, "tp", half)
    beside = [exchange(tokens, "tp", step) for step in near]
    own, *held = stage([tokens, *weights], own_rows * groups)
    across, own = lax.optimization_barrier((across, own))
    late = [exchange(across, "tp", step) for step in near]
    early_steps, late_steps = (0, *near, half), tuple(half + step for step in near)
    early = project([own, *beside, across], early_steps, held, heads)
    packed = finish(early[1], early_steps, late, late_steps, held, heads, groups, True)
    queries = finish(early[0], early_steps, late, late_steps, held, heads, groups, False)
    first, second = gather_pieces(packed, "sp")
    state = begin(queries, [], first, heads) if first else []
    if len(second) > 1:
        state, second = begin(queries, state, second[:1], heads), second[1:]
    rest = (mixing, head_gain, heads, groups)
    shares = attend(queries, state, second, *rest)
    last = groups - 1
    others = tuple(range(last - 1, 0, -1))
    farthest = exchange(shares[last], "tp", last)
    shares = [farthest] + [exchange(shares[step], "tp", step) for step in others] + [shares[0]]
    early = output([], [shares[-1], farthest], (0, last), out_weight, jnp.float32)
    return output([early], shares[1:-1], others, out_weight, jnp.bfloat16)


def solution(mesh):
    in_specs = (
        P(("sp", "tp"), None),
        P(None, "tp"),
        P(None, "tp"),
        P(None, "tp"),
        P(None, "tp"),
        P(None, "tp"),
        P("tp"),
        P(),
        P(),
    )
    out_specs = P(("sp", "tp"), None)
    return jax.shard_map(
        per_device, mesh=mesh, in_specs=in_specs, out_specs=out_specs, check_vma=False
    )
```

```python
import functools

import jax
import jax.numpy as jnp
import numpy as np
from jax import lax
from jax.experimental import pallas as pl
from jax.experimental.pallas import tpu as pltpu
from jax.sharding import PartitionSpec as P

HEAD = 64
GRID_W = 64
PAIR = 2 * HEAD

epsilon = 1e-06
theta_base = 10000.0
floor_value = -1e30
ring_limit = 16
chunk_rows = 1024
log2_e = 1.4426950408889634
MIB = 1 << 20
stage_grant = 52 * MIB

CONTRACT_LAST = (((1,), (1,)), ((), ()))


def turn_of(start, count):
    quarter = HEAD // 4
    lane = lax.broadcasted_iota(jnp.int32, (1, PAIR), 1)
    index = lane % quarter
    freqs = jnp.zeros((1, PAIR), jnp.float32)
    for j in range(quarter):
        freqs = jnp.where(index == j, theta_base ** (-j / quarter), freqs)
    token = start + lax.broadcasted_iota(jnp.int32, (count, PAIR), 0)
    by_row = (lane & (HEAD // 2)) == 0
    position = jnp.where(by_row, token // GRID_W, token % GRID_W).astype(jnp.float32)
    angle = position * freqs
    sine = jnp.sin(angle)
    return jnp.cos(angle), jnp.where((lane & quarter) == 0, -sine, sine)


def turned(field, cosine, sine):
    lane = lax.broadcasted_iota(jnp.int32, field.shape, 1)
    ahead = pltpu.roll(field, PAIR - HEAD // 4, 1)
    behind = pltpu.roll(field, HEAD // 4, 1)
    partner = jnp.where((lane & (HEAD // 4)) == 0, ahead, behind)
    return (field * cosine + partner * sine).astype(jnp.bfloat16)


def project_blocks(blocks, places, weight_refs, heads, q_ref, kv_ref, place):
    one_q, two_q, one_k, two_k, upper, lower, cosine_ref, sine_ref = weight_refs
    count = blocks[0].shape[0]
    tokens = jnp.concatenate([block[...] for block in blocks], axis=0)
    cosine, sine = [
        jnp.concatenate([ref[pl.ds(at, count), :] for at in places], axis=0)
        for ref in (cosine_ref, sine_ref)
    ]
    half = upper.shape[0]
    for head in range(heads):
        rows = slice(head * HEAD, (head + 1) * HEAD)
        columns = slice(head * PAIR, (head + 1) * PAIR)
        base = head * 2 * PAIR

        def turned_pair(first, second):
            joined = jnp.concatenate([first[rows, :], second[rows, :]], axis=0)
            pair = lax.dot_general(
                tokens, joined, CONTRACT_LAST, preferred_element_type=jnp.float32
            )
            return turned(pair, cosine, sine)

        if kv_ref is not None:
            kv_ref[place, base : base + PAIR] = turned_pair(one_k, two_k)
            values = jnp.dot(
                tokens[:, :half], upper[:, columns], preferred_element_type=jnp.float32
            ) + jnp.dot(tokens[:, half:], lower[:, columns], preferred_element_type=jnp.float32)
            kv_ref[place, base + PAIR : base + 2 * PAIR] = values.astype(jnp.bfloat16)
        if q_ref is not None:
            q_ref[place, columns] = turned_pair(one_q, two_q)


def place_of(step, count):
    return pl.multiple_of((lax.axis_index("tp") ^ step) * count, count)


def stage_kernel(count, *refs):
    sources, held, (cosine_ref, sine_ref, sems) = refs[:count], refs[count:-3], refs[-3:]
    half = sources[-1].shape[0] // 2
    sources = [*sources[:-1], sources[-1].at[pl.ds(0, half)], sources[-1].at[pl.ds(half, half)]]
    copies = [pltpu.make_async_copy(a, b, sems.at[i]) for i, (a, b) in enumerate(zip(sources, held))]
    for copy in copies:
        copy.start()
    rows = cosine_ref.shape[0]
    cosine_ref[...], sine_ref[...] = turn_of(lax.axis_index("sp") * rows, rows)
    for copy in copies:
        copy.wait()


def shapes_of(rows, heads):
    return [
        jax.ShapeDtypeStruct((rows, heads * PAIR), jnp.bfloat16),
        jax.ShapeDtypeStruct((rows, heads * 2 * PAIR), jnp.bfloat16),
    ]


def project_cost(rows, depth, heads):
    return pl.CostEstimate(
        flops=2 * rows * depth * heads * 3 * PAIR, bytes_accessed=0, transcendentals=0
    )


def stage(arrays, total):
    size = sum(a.size * 2 for a in arrays)
    rows, columns = arrays[-1].shape
    shapes = [a.shape for a in arrays[:-1]] + [(rows // 2, columns)] * 2
    return pl.pallas_call(
        functools.partial(stage_kernel, len(arrays)),
        out_shape=[jax.ShapeDtypeStruct(shape, arrays[0].dtype) for shape in shapes]
        + [jax.ShapeDtypeStruct((total, PAIR), jnp.float32)] * 2,
        in_specs=[pl.BlockSpec(memory_space=pltpu.HBM)] * len(arrays),
        scratch_shapes=[pltpu.SemaphoreType.DMA((len(shapes),))],
        cost_estimate=pl.CostEstimate(flops=size * 256, bytes_accessed=size, transcendentals=0),
        compiler_params=pltpu.CompilerParams(vmem_limit_bytes=stage_grant),
        name="stage",
    )(*arrays)


def project_kernel(heads, steps, *refs):
    blocks, refs = refs[: len(steps)], refs[len(steps) :]
    weight_refs, (q_ref, kv_ref) = refs[:8], refs[8:]
    places = [place_of(step, blocks[0].shape[0]) for step in steps]
    project_blocks(blocks, places, weight_refs, heads, q_ref, kv_ref, slice(None))


def project(blocks, steps, weights, heads):
    count, depth = blocks[0].shape
    rows = count * len(blocks)
    return pl.pallas_call(
        functools.partial(project_kernel, heads, steps),
        out_shape=shapes_of(rows, heads),
        cost_estimate=project_cost(rows, depth, heads),
        compiler_params=pltpu.CompilerParams(vmem_limit_bytes=8 * MIB),
        name="project",
    )(*blocks, *weights)


def finish_kernel(heads, steps, late_steps, keys, early_ref, *refs):
    blocks, refs = refs[: len(late_steps)], refs[len(late_steps) :]
    weight_refs, out_ref = refs[:8], refs[8]
    count = blocks[0].shape[0]
    for at, step in enumerate(steps):
        out_ref[pl.ds(place_of(step, count), count), :] = early_ref[at * count : (at + 1) * count, :]
    for step, block in zip(late_steps, blocks):
        place = place_of(step, count)
        project_blocks(
            [block],
            [place],
            weight_refs,
            heads,
            None if keys else out_ref,
            out_ref if keys else None,
            pl.ds(place, count),
        )


def finish(early, steps, blocks, late_steps, weights, heads, groups, keys):
    count, depth = blocks[0].shape
    return pl.pallas_call(
        functools.partial(finish_kernel, heads, steps, late_steps, keys),
        out_shape=jax.ShapeDtypeStruct((count * groups, early.shape[1]), early.dtype),
        cost_estimate=project_cost(count * len(blocks), depth, heads),
        compiler_params=pltpu.CompilerParams(vmem_limit_bytes=8 * MIB),
        name="keys" if keys else "queries",
    )(early, *blocks, *weights)


def both_of(pair):
    lane = lax.broadcasted_iota(jnp.int32, pair.shape, 1)
    nothing = jnp.zeros_like(pair)
    return jnp.concatenate(
        [jnp.where(lane < HEAD, pair, nothing), jnp.where(lane < HEAD, nothing, pair)], axis=0
    )


def lanes_of(scores):
    return [scores[:, at : at + PAIR] for at in range(0, scores.shape[1], PAIR)]


def absorb(state, both, kv_refs, head):
    scale = HEAD ** (-0.5) * log2_e
    base = head * 2 * PAIR

    def taken(carry, parts):
        scores = [
            lax.dot_general(
                both,
                ref[rows, base : base + PAIR],
                CONTRACT_LAST,
                preferred_element_type=jnp.float32,
            )
            for ref, rows in parts
        ]
        wide = functools.reduce(
            jnp.maximum, [part for s in scores for part in lanes_of(s)]
        )
        peak = jnp.broadcast_to(jnp.max(wide, axis=1, keepdims=True), wide.shape)
        total = summed = None
        if carry is not None:
            before, total, summed = carry
            peak = jnp.maximum(before, peak)
            factor = jnp.exp2((before - peak) * scale)
            total, summed = total * factor, summed * factor
        for s, (ref, rows) in zip(scores, parts):
            weights = [jnp.exp2((part - peak) * scale) for part in lanes_of(s)]
            partial = functools.reduce(jnp.add, weights)
            product = jnp.dot(
                jnp.concatenate([w.astype(jnp.bfloat16) for w in weights], axis=1),
                ref[rows, base + PAIR : base + 2 * PAIR],
                preferred_element_type=jnp.float32,
            )
            total = partial if total is None else total + partial
            summed = product if summed is None else summed + product
        return peak, total, summed

    if sum(ref.shape[0] for ref in kv_refs) <= chunk_rows:
        return taken(state, [(ref, slice(None)) for ref in kv_refs])
    for ref in kv_refs:
        size = np.gcd(ref.shape[0], chunk_rows).item()
        if state is None:
            rows = both.shape[0]
            state = (
                jnp.full((rows, PAIR), floor_value, jnp.float32),
                jnp.zeros((rows, PAIR), jnp.float32),
                jnp.zeros((rows, PAIR), jnp.float32),
            )

        def step(index, carry, ref=ref, size=size):
            return taken(carry, [(ref, pl.ds(pl.multiple_of(index * size, size), size))])

        state = lax.fori_loop(0, ref.shape[0] // size, step, state)
    return state


def begin_kernel(heads, pieces, held, q_ref, *refs):
    state_refs, kv_refs, out_refs = refs[:held], refs[held : held + pieces], refs[held + pieces :]
    for head in range(heads):
        state = tuple(ref[head] for ref in state_refs) or None
        both = both_of(q_ref[:, head * PAIR : (head + 1) * PAIR])
        for ref, value in zip(out_refs, absorb(state, both, kv_refs, head)):
            ref[head] = value


def attend_kernel(heads, pieces, held, groups, q_ref, *refs):
    state_refs, refs = refs[:held], refs[held:]
    kv_refs, (mixing_ref, gain_ref), out_refs = refs[:pieces], refs[pieces : pieces + 2], refs[pieces + 2 :]
    total_rows = q_ref.shape[0]
    share = total_rows // groups
    rows = total_rows
    places = [place_of(step, share) for step in range(groups)]
    for head in range(heads):
        columns = slice(head * PAIR, (head + 1) * PAIR)
        pair = jnp.concatenate([q_ref[pl.ds(at, share), columns] for at in places], axis=0)
        state = None
        if held:
            spots = places + [total_rows + at for at in places]
            state = tuple(
                jnp.concatenate([ref[head, pl.ds(at, share), :] for at in spots], axis=0)
                for ref in state_refs
            )
        _, total, summed = absorb(state, both_of(pair), kv_refs, head)
        ratio = summed / jnp.sum(total, axis=1, keepdims=True)
        mixed = ratio[:rows] - mixing_ref[:, head : head + 1] * ratio[rows:]
        square = jnp.mean(mixed * mixed, axis=1, keepdims=True)
        normed = (mixed * lax.rsqrt(square + epsilon) * gain_ref[...]).astype(jnp.bfloat16)
        for at, out_ref in enumerate(out_refs):
            out_ref[:, columns] = normed[at * share : (at + 1) * share]


def attend_grant(rows, keys, heads):
    return 4 * rows * min(keys, chunk_rows) * 8 + 2 * keys * heads * 2 * PAIR + 8 * MIB


def attend_cost(rows, keys, heads):
    return pl.CostEstimate(
        flops=2 * 4 * rows * keys * heads * PAIR,
        bytes_accessed=0,
        transcendentals=2 * rows * keys * heads,
    )


def begin(queries, state, pieces, heads):
    rows = queries.shape[0]
    keys = sum(p.shape[0] for p in pieces)
    return pl.pallas_call(
        functools.partial(begin_kernel, heads, len(pieces), len(state)),
        out_shape=[
            jax.ShapeDtypeStruct((heads, 2 * rows, PAIR), jnp.float32)
        ]
        * 3,
        cost_estimate=attend_cost(rows, keys, heads),
        compiler_params=pltpu.CompilerParams(vmem_limit_bytes=attend_grant(rows, keys, heads)),
        name="middle" if state else "begin",
    )(queries, *state, *pieces)


def attend(queries, state, pieces, mixing, gain, heads, groups):
    rows = queries.shape[0]
    keys = sum(p.shape[0] for p in pieces)
    share = jax.ShapeDtypeStruct((rows // groups, heads * PAIR), jnp.bfloat16)
    return pl.pallas_call(
        functools.partial(attend_kernel, heads, len(pieces), len(state), groups),
        out_shape=[share] * groups,
        cost_estimate=attend_cost(rows, keys, heads),
        compiler_params=pltpu.CompilerParams(vmem_limit_bytes=attend_grant(rows, keys, heads)),
        name="attend",
    )(queries, *state, *pieces, mixing.reshape(1, heads), gain.reshape(1, PAIR))


def summed_shares(share_refs, steps, weight_ref, total):
    width = share_refs[0].shape[1]
    for step, ref in zip(steps, share_refs):
        part = jnp.dot(
            ref[...],
            weight_ref[pl.ds(place_of(step, width), width), :],
            preferred_element_type=jnp.float32,
        )
        total = part if total is None else total + part
    return total


def output_kernel(steps, held, *refs):
    share_refs, weight_ref, out_ref = refs[held : held + len(steps)], refs[-2], refs[-1]
    total = summed_shares(share_refs, steps, weight_ref, refs[0][...] if held else None)
    out_ref[...] = total.astype(out_ref.dtype)


def output(earlier, shares, steps, weight, dtype):
    rows, width = shares[0].shape
    return pl.pallas_call(
        functools.partial(output_kernel, steps, len(earlier)),
        out_shape=jax.ShapeDtypeStruct((rows, weight.shape[1]), dtype),
        cost_estimate=pl.CostEstimate(
            flops=2 * rows * width * len(steps) * weight.shape[1],
            bytes_accessed=0,
            transcendentals=0,
        ),
        compiler_params=pltpu.CompilerParams(vmem_limit_bytes=8 * MIB),
        name="output" if earlier else "early",
    )(*earlier, *shares, weight)


def exchange(block, axis, step):
    size = lax.axis_size(axis)
    return lax.ppermute(block, axis, [(i, i ^ step) for i in range(size)])


def gather_pieces(packed, axis):
    size = lax.axis_size(axis)
    if size > ring_limit or size & (size - 1):
        return [], [lax.all_gather(packed, axis, axis=0, tiled=True)]
    half = size // 2
    far = exchange(packed, axis, half)
    near = [exchange(packed, axis, step) for step in range(half - 1, 0, -1)]
    forwarded = [exchange(far, axis, step) for step in range(half - 1, 0, -1)]
    return [packed, far] + near, forwarded


def per_device(
    tokens, query_one, query_two, key_one, key_two, value_weight, mixing, out_weight, head_gain
):
    groups = lax.axis_size("tp")
    own_rows = tokens.shape[0]
    heads = query_one.shape[1] // HEAD
    weights = (query_one.T, query_two.T, key_one.T, key_two.T, value_weight)
    half = groups // 2
    near = tuple(range(1, half))
    across = exchange(tokens, "tp", half)
    beside = [exchange(tokens, "tp", step) for step in near]
    own, *held = stage([tokens, *weights], own_rows * groups)
    across, own = lax.optimization_barrier((across, own))
    late = [exchange(across, "tp", step) for step in near]
    early_steps, late_steps = (0, *near, half), tuple(half + step for step in near)
    early = project([own, *beside, across], early_steps, held, heads)
    packed = finish(early[1], early_steps, late, late_steps, held, heads, groups, True)
    queries = finish(early[0], early_steps, late, late_steps, held, heads, groups, False)
    first, second = gather_pieces(packed, "sp")
    state = begin(queries, [], first, heads) if first else []
    while len(second) > 1:
        state, second = begin(queries, state, second[:1], heads), second[1:]
    rest = (mixing, head_gain, heads, groups)
    shares = attend(queries, state, second, *rest)
    last = groups - 1
    farthest = exchange(shares[last], "tp", last)
    others = [exchange(shares[step], "tp", step) for step in range(last - 1, 1, -1)]
    closest = exchange(shares[1], "tp", 1)
    early = output([], [shares[0], farthest, closest], (0, last, 1), out_weight, jnp.float32)
    return output([early], others, tuple(range(last - 1, 1, -1)), out_weight, jnp.bfloat16)


def solution(mesh):
    in_specs = (
        P(("sp", "tp"), None),
        P(None, "tp"),
        P(None, "tp"),
        P(None, "tp"),
        P(None, "tp"),
        P(None, "tp"),
        P("tp"),
        P(),
        P(),
    )
    out_specs = P(("sp", "tp"), None)
    return jax.shard_map(
        per_device, mesh=mesh, in_specs=in_specs, out_specs=out_specs, check_vma=False
    )
```
